256 devices in a mesh: grp: 2 (over y), sp: 32 (over z, core), tp: 4 (over x).
Axes of the slice: x: 4, y: 2, z: 16, core: 2. Of those that a mesh axis runs over, the one named last changes fastest.
The devices are a block of a 4x16x16 slice.
Arguments:
- residual_in: bfloat16 [16384, 2048], P(('grp', 'sp', 'tp')), parts along dimension 0, may hold values from -6 to 6
- query_rows: bfloat16 [16384, 2048], P(('grp', 'sp'), 'tp'), parts along dimension 0, may hold values from -6 to 6
- key_rows: bfloat16 [16384, 512], P(('grp', 'sp'), 'tp'), parts along dimension 0, may hold values from -6 to 6
- value_rows: bfloat16 [16384, 512], P(('grp', 'sp'), 'tp'), parts along dimension 0, may hold values from -6 to 6
- forget_cumsum: float32 [16384, 16], P(('grp', 'sp'), 'tp'), parts along dimension 0, as said below
- head_gain: float32 [2048], P('tp'), may hold values from 0.1 to 1.9
- w_out: bfloat16 [2048, 2048], P('tp'), may hold values from -0.125 to 0.125
- w_up: bfloat16 [2048, 8192], P('sp', 'tp'), may hold values from -0.125 to 0.125
- w_down: bfloat16 [8192, 2048], P('tp', 'sp'), may hold values from -0.0625 to 0.0625
- mixer_gain: float32 [2048], replicated, may hold values from 0.1 to 1.9
- channel_gain: float32 [2048], replicated, may hold values from 0.1 to 1.9
Outputs:
- layer_out: bfloat16 [16384, 2048], P(('grp', 'sp', 'tp')), parts along dimension 0
The draws below stay inside these ranges and needn't reach their ends.
There are 2 independent parts, one for each index of `grp`. The reference program is written for one: setup_inputs(seed, part) draws one part's arguments, and reference() takes and returns one part's arrays. A program takes and returns all parts, laid end to end along the dimension named above; an argument that names none is the same for every part. Nothing has to cross between parts.
Inputs may be any that keep to these rules, and one draw needn't show every extreme that they name: `forget_cumsum`: Non-positive; along the positions, each head's entries never rise.
All inputs are finite; a program needn't handle non-finite values.
Results may differ from the reference program's by a relative error of at most 0.015.
Values may be sent and summed in bfloat16 or wider, within the bound.
A program may use at most 128 MiB of HBM per device.

```python
import jax
import jax.numpy as jnp
from jax import lax

D = 2048
QUERY_HEADS = 16
KV_HEADS = 4
HD = 128
FF = 8192
TOK_DEV = 256
SEQUENCE_TOKENS = 8192


def draw_key_rows(key, part):
    drawn = jax.random.normal(jax.random.fold_in(key, 21), (SEQUENCE_TOKENS, KV_HEADS * HD), jnp.float32)
    drawn = jnp.clip(drawn, -6.0, 6.0)
    return drawn.astype(jnp.bfloat16)


def draw_query_rows(key, part):
    drawn = jax.random.normal(jax.random.fold_in(key, 22), (SEQUENCE_TOKENS, QUERY_HEADS * HD), jnp.float32)
    drawn = jnp.clip(drawn, -6.0, 6.0)
    return drawn.astype(jnp.bfloat16)


def draw_forget_cumsum(key, part):
    residual_paths = [jax.random.fold_in(key, 30 + offset) for offset in range(7)]
    slow_share = 0.5
    sluggish_part = jax.random.uniform(residual_paths[0], (QUERY_HEADS,)) < slow_share
    slow_total = jax.random.uniform(residual_paths[1], (QUERY_HEADS,), minval=0.1, maxval=0.5)
    fast_rate = 1.0 / jax.random.uniform(residual_paths[2], (QUERY_HEADS,), minval=30.0, maxval=100.0)
    rate = jnp.where(sluggish_part, slow_total / SEQUENCE_TOKENS, fast_rate)
    position = jnp.arange(SEQUENCE_TOKENS, dtype=jnp.float32)
    ramp = 0.5 + position / SEQUENCE_TOKENS
    block_factor = jnp.exp(jax.random.uniform(residual_paths[3], (SEQUENCE_TOKENS // TOK_DEV,), minval=-0.7, maxval=0.7))
    block_factor = jnp.repeat(block_factor, TOK_DEV)
    rough = jax.random.uniform(residual_paths[4], (SEQUENCE_TOKENS, QUERY_HEADS), minval=0.2, maxval=1.8)
    gate_logarithm = -rate[None, :] * (ramp * block_factor)[:, None] * rough
    spike_position = jax.random.randint(residual_paths[5], (3,), 0, SEQUENCE_TOKENS)
    spike_penalty = jax.random.uniform(residual_paths[6], (3, QUERY_HEADS), minval=0.2, maxval=0.5)
    matched_rows = (jnp.arange(SEQUENCE_TOKENS)[:, None] == spike_position[None, :]).astype(jnp.float32)
    spike_pattern = jnp.dot(matched_rows, jnp.log(1.0 - spike_penalty))
    gate_logarithm = gate_logarithm + jnp.where(sluggish_part[None, :], spike_pattern, 0.0)
    return jnp.cumsum(gate_logarithm, axis=0).astype(jnp.float32)


def steps_of(stream_key, shape, cuts, least, largest):
    loudness, own = 1.0, jax.random.fold_in(stream_key, 6)
    for dim, shards_of in cuts:
        draws = jnp.exp(jax.random.uniform(jax.random.fold_in(own, dim), (shards_of,), jnp.float32, least / len(cuts), largest / len(cuts)))
        loudness = loudness * jnp.repeat(draws, shape[dim] // shards_of).reshape([-1 if axis == dim else 1 for axis in range(len(shape))])
    return loudness


def scatter_about(own_key, extent, width, most, pieces=(), held_as=jnp.bfloat16):
    values = width * jax.random.normal(own_key, extent, jnp.float32)
    if pieces:
        values = values * steps_of(own_key, extent, pieces, -0.22, 0.18)
    return jnp.clip(values, -most, most).astype(held_as)


def setup_inputs(seed: int = 0, part: int = 0) -> dict:
    splits = jax.random.split(jax.random.key(seed), 12)
    own_keys = jax.random.split(jax.random.fold_in(splits[11], part), 12)
    residual_in = scatter_about(own_keys[0], (SEQUENCE_TOKENS, D), 1.0, 6.0, ((0, 128),))
    query_rows = draw_query_rows(jax.random.fold_in(jax.random.fold_in(splits[11], part), 71), part)
    key_rows = draw_key_rows(jax.random.fold_in(jax.random.fold_in(splits[11], part), 71), part)
    value_rows = scatter_about(own_keys[3], (SEQUENCE_TOKENS, KV_HEADS * HD), 1.0, 6.0, ((0, 32), (1, 4)))
    forget_cumsum = draw_forget_cumsum(jax.random.fold_in(jax.random.fold_in(splits[11], part), 71), part)
    head_gain = jnp.clip(1.0 + 0.18 * jax.random.normal(splits[5], (QUERY_HEADS * HD,), jnp.float32), 0.1, 1.9)
    w_out = scatter_about(splits[6], (QUERY_HEADS * HD, D), (QUERY_HEADS * HD) ** -0.5, 0.125, ((0, 4),))
    w_up = scatter_about(splits[7], (D, FF), D ** -0.5, 0.125, ((0, 32), (1, 4)))
    w_down = scatter_about(splits[8], (FF, D), FF ** -0.5, 0.0625, ((0, 4), (1, 32)))
    mixer_gain = jnp.clip(1.0 + 0.18 * jax.random.normal(splits[9], (D,), jnp.float32), 0.1, 1.9)
    channel_gain = jnp.clip(1.0 + 0.18 * jax.random.normal(splits[10], (D,), jnp.float32), 0.1, 1.9)
    return {"residual_in": residual_in, "query_rows": query_rows, "key_rows": key_rows, "value_rows": value_rows, "forget_cumsum": forget_cumsum, "head_gain": head_gain, "w_out": w_out, "w_up": w_up, "w_down": w_down, "mixer_gain": mixer_gain, "channel_gain": channel_gain}


ALPHA = 8.0 ** 0.25
EPSILON = 1e-05
NEG_FILL = -1e+30

def layer_scale(inputs, gain_vec):
    centered = inputs - lax.optimization_barrier(jnp.mean(inputs, axis=-1, keepdims=True))
    variance = lax.optimization_barrier(jnp.mean(centered * centered, axis=-1, keepdims=True))
    return centered * lax.rsqrt(variance + EPSILON) * gain_vec

def reference(residual_in, query_rows, key_rows, value_rows, forget_cumsum, head_gain, w_out, w_up, w_down, mixer_gain, channel_gain):
    group_size = QUERY_HEADS // KV_HEADS
    block_rows = 512 if SEQUENCE_TOKENS % 512 == 0 else SEQUENCE_TOKENS
    block_count = SEQUENCE_TOKENS // block_rows
    score_scale = HD ** (-0.5)
    key_full = key_rows.astype(jnp.float32).reshape(SEQUENCE_TOKENS, KV_HEADS, HD)
    value_full = value_rows.astype(jnp.float32).reshape(SEQUENCE_TOKENS, KV_HEADS, HD)
    gate_keys = forget_cumsum.reshape(SEQUENCE_TOKENS, KV_HEADS, group_size).transpose(1, 2, 0)
    key_pos = jnp.arange(SEQUENCE_TOKENS, dtype=jnp.int32)

    def attend(block_index):
        first_row = (block_index * block_rows).astype(jnp.int32)
        query_full = lax.dynamic_slice_in_dim(query_rows, first_row, block_rows, 0).astype(jnp.float32)
        query_full = query_full.reshape(block_rows, KV_HEADS, group_size, HD)
        gate_rows = lax.dynamic_slice_in_dim(forget_cumsum, first_row, block_rows, 0)
        gate_rows = gate_rows.reshape(block_rows, KV_HEADS, group_size).transpose(1, 2, 0)
        scores = jnp.einsum('tkgd,ukd->kgtu', query_full, key_full) * score_scale
        scores = scores + gate_rows[..., None] - gate_keys[:, :, None, :]
        query_pos = first_row + jnp.arange(block_rows, dtype=jnp.int32)
        allowed = key_pos[None, :] <= query_pos[:, None]
        scores = jnp.where(allowed, scores, NEG_FILL)
        peak_score = lax.optimization_barrier(jnp.max(scores, axis=-1, keepdims=True))
        weights = jnp.exp(scores - peak_score)
        denom_sum = lax.optimization_barrier(jnp.sum(weights, axis=-1))
        rounded = lax.optimization_barrier(weights.astype(jnp.bfloat16)).astype(jnp.float32)
        attended = jnp.einsum('kgtu,ukd->kgtd', rounded, value_full) / denom_sum[..., None]
        normed = attended * lax.rsqrt(lax.optimization_barrier(jnp.mean(attended * attended, axis=-1, keepdims=True)) + EPSILON)
        normed = normed * head_gain.reshape(KV_HEADS, group_size, 1, HD)
        return normed.transpose(2, 0, 1, 3).reshape(block_rows, QUERY_HEADS * HD).astype(jnp.bfloat16)
    heads_out = lax.map(attend, jnp.arange(block_count, dtype=jnp.int32)).reshape(SEQUENCE_TOKENS, QUERY_HEADS * HD)
    branch = jnp.dot(heads_out, w_out, preferred_element_type=jnp.float32)
    mid = layer_scale(ALPHA * residual_in.astype(jnp.float32) + branch, mixer_gain).astype(jnp.bfloat16)
    lifted = jnp.dot(mid, w_up, preferred_element_type=jnp.float32)
    active = jnp.square(jax.nn.relu(lifted)).astype(jnp.bfloat16)
    lowered = jnp.dot(active, w_down, preferred_element_type=jnp.float32)
    return layer_scale(ALPHA * mid.astype(jnp.float32) + lowered, channel_gain).astype(jnp.bfloat16)
```

```python
import functools

import jax
import jax.numpy as jnp
from jax import lax
from jax.experimental import pallas as pl
from jax.experimental.pallas import tpu as pltpu
from jax.sharding import PartitionSpec as P

HD = 128
ALPHA = 8.0**0.25
EPSILON = 1e-05
NEG_FILL = -1e30
LOG2E = 1.4426950408889634
MESH = pl.DeviceIdType.MESH
F32 = jnp.float32
BF16 = jnp.bfloat16

KV, GATE, UP, DOWN = 0, 1, 2, 3


def dot_nt(a, b):
    return lax.dot_general(a, b, (((1,), (1,)), ((), ())), preferred_element_type=F32)


def dot_nn(a, b):
    return lax.dot_general(a, b, (((1,), (0,)), ((), ())), preferred_element_type=F32)


def layer_kernel(
    chips,
    q_hbm, k_hbm, v_hbm, f_hbm, res_ref, hgain_ref, wo_hbm, wu_hbm, wd_hbm, mgain_ref, cgain_ref,
    out_ref,
    q_s, kv, gate, wo_s, wu, wd_raw, wd, acc, m_s, l_s, heads, bp, b1, b2t, b2, mid, act,
    dp, d1, d2t, d2, d3t, d3, keep, low,
    ring_send, ring_recv, twin_send, twin_recv, local, bx_send, bx_recv, mx_send, mx_recv,
    dx_send, dx_recv,
):
    far = chips // 2
    grp, sp, tp = lax.axis_index("grp"), lax.axis_index("sp"), lax.axis_index("tp")
    z, core = sp // 2, sp % 2
    pair = grp % 2
    rows = q_s.shape[1]
    ffh = act.shape[1]
    right = (grp, ((z + 1) % chips) * 2 + core, tp)
    left = (grp, ((z + chips - 1) % chips) * 2 + core, tp)
    twin = (grp, z * 2 + 1 - core, tp)
    xa = tp + 1 - 2 * (tp % 2)
    xb = 3 - tp
    dev_a, dev_b = (grp, sp, xa), (grp, sp, xb)
    dev_y = (grp + 1 - 2 * pair, sp, tp)
    peers = (right, left, twin, dev_a, dev_b, dev_y)
    bufs = (kv, gate, wu, wd)

    def remote(src, dst, ss, rs, dev):
        return pltpu.make_async_remote_copy(
            src_ref=src, dst_ref=dst, send_sem=ss, recv_sem=rs, device_id=dev, device_id_type=MESH
        )

    def when(cond, fn):
        if isinstance(cond, bool):
            if cond:
                fn()
        else:
            pl.when(cond)(fn)

    def both(a, b):
        return (a and b) if isinstance(a, bool) and isinstance(b, bool) else jnp.logical_and(a, b)

    def ring_copy(st, way, slot, s):
        buf = bufs[st].at[slot]
        return remote(buf, buf, ring_send.at[st, way], ring_recv.at[st, way, s], right if way == 0 else left)

    def twin_copy(st, way, slot, s):
        buf = bufs[st].at[slot]
        return remote(buf, buf, twin_send.at[st, way], twin_recv.at[st, way, s], twin)

    def chip_at(way, s):
        return (z + chips - s) % chips if way == 0 else (z + s) % chips

    def ring_begin(st):
        ring_copy(st, 0, sp, 1).start()
        ring_copy(st, 1, sp, 1).start()
        twin_copy(st, 0, sp, 0).start()

    def ring_step(st, s):
        def one(way, last):
            slot = chip_at(way, s) * 2 + core
            ring_copy(st, way, slot, s).wait_recv()
            ring_copy(st, way, slot, s).wait_send()

            when(s < last, lambda: ring_copy(st, way, slot, s + 1).start())
            when(way == 0 or s > 1, lambda: twin_copy(st, way, slot, s).wait_send())
            twin_copy(st, way, slot, s).start()

        one(0, far)
        when(s < far, lambda: one(1, far - 1))

    def twin_wait(st, s):
        twin_copy(st, 0, chip_at(0, s) * 2 + 1 - core, s).wait_recv()
        when(
            both(s > 0, s < far),
            lambda: twin_copy(st, 1, chip_at(1, s) * 2 + 1 - core, s).wait_recv(),
        )

    def ring_end(st):
        twin_copy(st, 0, sp, 0).wait_send()
        twin_copy(st, 1, sp, 0).wait_send()

    loads = [
        pltpu.make_async_copy(k_hbm, kv.at[sp, 0], local.at[0]),
        pltpu.make_async_copy(v_hbm, kv.at[sp, 1], local.at[1]),
        pltpu.make_async_copy(f_hbm, gate.at[sp], local.at[2]),
        pltpu.make_async_copy(wu_hbm.at[:, pl.ds(pl.multiple_of(pair * ffh, ffh), ffh)], wu.at[sp], local.at[3]),
        pltpu.make_async_copy(wd_hbm.at[pl.ds(pl.multiple_of(pair * ffh, ffh), ffh)], wd_raw, local.at[4]),
        pltpu.make_async_copy(wo_hbm, wo_s, local.at[5]),
    ]
    loads += [pltpu.make_async_copy(q_hbm.at[:, pl.ds(h * HD, HD)], q_s.at[h], local.at[6 + h]) for h in range(4)]
    for c in loads:
        c.start()

    barrier = pltpu.get_barrier_semaphore()
    for dev in peers:
        pl.semaphore_signal(barrier, inc=1, device_id=dev, device_id_type=MESH)
    pl.semaphore_wait(barrier, len(peers))

    for c in loads[:3]:
        c.wait()
    ring_begin(KV)
    ring_begin(GATE)

    gate_base = [None] * 4
    own_gate = gate[sp]
    for h in range(4):
        gate_base[h] = own_gate[h : h + 1, 0:1]

    def scores(h, src):
        s = dot_nt(q_s[h], kv[src, 0])
        bias = (gate_base[h] - gate[src][h : h + 1, :]) * LOG2E
        return s * (HD**-0.5 * LOG2E) + bias

    def spread(col):
        return jnp.broadcast_to(col, (rows, HD))

    for c in loads[6:]:
        c.wait()
    causal = lax.broadcasted_iota(jnp.int32, (rows, rows), 1) <= lax.broadcasted_iota(jnp.int32, (rows, rows), 0)
    for h in range(4):
        s = jnp.where(causal, scores(h, sp), NEG_FILL)
        m = spread(jnp.max(s, axis=1, keepdims=True))
        p = jnp.exp2(s - jnp.concatenate([m] * (rows // HD), axis=1))
        m_s[h] = m
        l_s[h] = spread(jnp.sum(p, axis=1, keepdims=True))
        acc[h] = dot_nn(p.astype(BF16), kv[sp, 1])

    def attend(srcs):
        for h in range(4):
            ss = [scores(h, src) for src in srcs]
            top = functools.reduce(jnp.maximum, ss)
            m_old = m_s[h]
            m = jnp.maximum(m_old, spread(jnp.max(top, axis=1, keepdims=True)))
            wide = jnp.concatenate([m] * (rows // HD), axis=1)
            ps = [jnp.exp2(s - wide) for s in ss]
            fade = jnp.exp2(m_old - m)
            total = functools.reduce(jnp.add, ps)
            m_s[h] = m
            l_s[h] = l_s[h] * fade + spread(jnp.sum(total, axis=1, keepdims=True))
            out = dot_nn(ps[0].astype(BF16), kv[srcs[0], 1])
            for p, src in zip(ps[1:], srcs[1:]):
                out = out + dot_nn(p.astype(BF16), kv[src, 1])
            acc[h] = acc[h] * fade + out

    def attend_step(s):
        @pl.when(z - s >= 0)
        def _():
            c = chip_at(0, s) * 2
            attend([c, c + 1])

        @pl.when(both(s < far, z + s >= chips) if not isinstance(s, int) else jnp.logical_and(z + s >= chips, s < far))
        def _():
            c = chip_at(1, s) * 2
            attend([c, c + 1])

    def kv_step(s, carry):
        ring_step(KV, s)
        ring_step(GATE, s)
        twin_wait(KV, s - 1)
        twin_wait(GATE, s - 1)

        @pl.when(jnp.logical_and(s == 1, core == 1))
        def _():
            attend([sp - 1])

        @pl.when(s > 1)
        def _():
            attend_step(s - 1)

        return carry

    lax.fori_loop(1, far + 1, kv_step, 0)
    loads[3].wait()
    ring_begin(UP)
    twin_wait(KV, far)
    twin_wait(GATE, far)
    attend_step(far)
    ring_end(KV)
    ring_end(GATE)

    loads[4].wait()
    cols = wd_raw.shape[1]
    eye = (
        lax.broadcasted_iota(jnp.int32, (cols, cols), 0) == lax.broadcasted_iota(jnp.int32, (cols, cols), 1)
    ).astype(BF16)
    wd[sp] = dot_nt(eye, wd_raw[...]).astype(BF16)

    loads[5].wait()
    for h in range(4):
        att = acc[h] / l_s[h]
        norm = lax.rsqrt(jnp.mean(att * att, axis=1, keepdims=True) + EPSILON)
        heads[:, h * HD : (h + 1) * HD] = (att * norm * hgain_ref[h : h + 1, :]).astype(BF16)
    half = bp.shape[3]
    own = bp.shape[2]
    for j in range(4):
        w = half // 2
        part = dot_nn(heads[...], wo_s[:, j * w : (j + 1) * w]).astype(BF16)
        bp[j // 2, :, :, (j % 2) * w : (j % 2 + 1) * w] = part.reshape(4, own, w)

    far_a = 3 - xa
    first = (dev_a, dev_b)
    second = (dev_b, dev_a)
    first_x = (xa, xb)
    second_x = (xb, xa)

    def b1_copy(hf, j):
        src = bp.at[hf, first_x[hf] if j == 0 else far_a]
        return remote(src, b1.at[hf, j], bx_send.at[hf, j], bx_recv.at[hf, j], first[hf])

    def b2_copy(hf):
        return remote(b2t.at[hf], b2.at[hf], bx_send.at[hf, 2], bx_recv.at[hf, 2], second[hf])

    for hf in range(2):
        b1_copy(hf, 1).start()
    for hf in range(2):
        b1_copy(hf, 0).start()
    ring_step(UP, 1)
    for hf in range(2):
        b1_copy(hf, 1).wait_recv()
        b2t[hf] = (bp[hf, second_x[hf]].astype(F32) + b1[hf, 1].astype(F32)).astype(BF16)
        b2_copy(hf).start()
    ring_step(UP, 2)
    sums = []
    for hf in range(2):
        b1_copy(hf, 0).wait_recv()
    ring_step(UP, 3)
    for hf in range(2):
        b2_copy(hf).wait_recv()
        part = bp[hf, tp].astype(F32) + b1[hf, 0].astype(F32) + b2[hf].astype(F32)
        sums.append(ALPHA * res_ref[:, hf * half : (hf + 1) * half].astype(F32) + part)

    def layer_norm(parts, gain_ref):
        width = 2 * half
        mean = sum(jnp.sum(p, axis=1, keepdims=True) for p in parts) * (1.0 / width)
        parts = [p - mean for p in parts]
        var = sum(jnp.sum(p * p, axis=1, keepdims=True) for p in parts) * (1.0 / width)
        inv = lax.rsqrt(var + EPSILON)
        return [
            (p * inv * gain_ref[:, i * half : (i + 1) * half]).astype(BF16) for i, p in enumerate(parts)
        ]

    for hf, part in enumerate(layer_norm(sums, mgain_ref)):
        mid[hf, tp, pair] = part

    def my_copy(hf):
        return remote(mid.at[hf, tp, pair], mid.at[hf, tp, pair], mx_send.at[hf, 0], mx_recv.at[hf, 0], dev_y)

    def m1_copy(hf, j):
        ref = mid.at[hf, tp, pair if j == 0 else 1 - pair]
        return remote(ref, ref, mx_send.at[hf, 1 + j], mx_recv.at[hf, 1 + j], first[hf])

    def m2_copy(hf, j):
        ref = mid.at[hf, tp if j == 0 else first_x[hf]]
        return remote(ref, ref, mx_send.at[hf, 3 + j], mx_recv.at[hf, 3 + j], second[hf])

    for hf in range(2):
        my_copy(hf).start()
        m1_copy(hf, 0).start()
    ring_step(UP, 4)
    for hf in range(2):
        my_copy(hf).wait_recv()
        m1_copy(hf, 1).start()
        m2_copy(hf, 0).start()
    ring_step(UP, 5)
    ring_step(UP, 6)
    for hf in range(2):
        m1_copy(hf, 0).wait_recv()
        m1_copy(hf, 1).wait_recv()
        m2_copy(hf, 1).start()
    ring_step(UP, 7)
    ring_step(UP, 8)
    ring_begin(DOWN)
    for s in range(far + 1):
        twin_wait(UP, s)
    ring_step(DOWN, 1)
    ring_step(DOWN, 2)
    for hf in range(2):
        m2_copy(hf, 0).wait_recv()
        m2_copy(hf, 1).wait_recv()
    ring_end(UP)

    toks = act.shape[0]
    tile = 256

    def up_tile(j, carry):
        cs = pl.ds(pl.multiple_of(j * tile, tile), tile)
        total = None
        for hf in range(2):
            blocks = wu.shape[0] // 2
            w = wu[hf * blocks : (hf + 1) * blocks, :, cs].reshape(half, tile)
            part = dot_nn(mid[hf].reshape(toks, half), w)
            total = part if total is None else total + part
        pos = jnp.maximum(total, 0.0)
        act[:, cs] = (pos * pos).astype(BF16)
        return carry

    lax.fori_loop(0, ffh // tile // 2, up_tile, 0)
    ring_step(DOWN, 3)
    lax.fori_loop(ffh // tile // 2, ffh // tile, up_tile, 0)
    early = 3

    wide = 2 * cols

    def chunk_chip(t, hf):
        return jnp.where(t == far, z, chip_at(0, t)) if hf == 0 else jnp.where(t == far, chip_at(0, t), chip_at(1, t))

    def d1_copy(t, hf, j):
        src = dp.at[t - 1, hf, first_x[hf] if j == 0 else far_a]
        return remote(src, d1.at[t - 1, hf, j], dx_send.at[t - 1, hf, j], dx_recv.at[t - 1, hf, j], first[hf])

    def d2_copy(t, hf):
        return remote(
            d2t.at[t - 1, hf], d2.at[t - 1, hf], dx_send.at[t - 1, hf, 2], dx_recv.at[t - 1, hf, 2], second[hf]
        )

    def d3_copy(t, hf):
        return remote(
            d3t.at[t - 1, hf], d3.at[t - 1, hf], dx_send.at[t - 1, hf, 3], dx_recv.at[t - 1, hf, 3], dev_y
        )

    def down_step(i, carry):
        @pl.when(jnp.logical_and(i > early, i <= far))
        def _():
            ring_step(DOWN, i)

        @pl.when(jnp.logical_and(i >= 2, i <= far + 1))
        def _():
            t = i - 1
            twin_wait(DOWN, t)

            @pl.when(t == far)
            def _():
                twin_wait(DOWN, 0)

            w = jnp.concatenate(
                [wd[pl.ds(chunk_chip(t, hf) * 2, 2)].reshape(wide, ffh) for hf in range(2)], axis=0
            )
            part = dot_nt(act[...], w).astype(BF16)
            for hf in range(2):
                dp[t - 1, hf] = part[:, hf * wide : (hf + 1) * wide].reshape(4, 2, own, wide)
                d1_copy(t, hf, 1).start()
                d1_copy(t, hf, 0).start()

        @pl.when(jnp.logical_and(i >= 3, i <= far + 2))
        def _():
            t = i - 2
            for hf in range(2):
                d1_copy(t, hf, 1).wait_recv()
                d2t[t - 1, hf] = (
                    dp[t - 1, hf, second_x[hf]].astype(F32) + d1[t - 1, hf, 1].astype(F32)
                ).astype(BF16)
                d2_copy(t, hf).start()

        @pl.when(jnp.logical_and(i >= 4, i <= far + 3))
        def _():
            t = i - 3
            for hf in range(2):
                d1_copy(t, hf, 0).wait_recv()
                d2_copy(t, hf).wait_recv()

                def whole(y):
                    return (
                        dp[t - 1, hf, tp, y].astype(F32)
                        + d1[t - 1, hf, 0, y].astype(F32)
                        + d2[t - 1, hf, y].astype(F32)
                    )

                d3t[t - 1, hf] = whole(1 - pair).astype(BF16)
                d3_copy(t, hf).start()
                keep[t - 1, hf] = whole(pair)

        @pl.when(i >= 5)
        def _():
            t = i - 4
            for hf in range(2):
                d3_copy(t, hf).wait_recv()
                cs = pl.ds(pl.multiple_of(chunk_chip(t, hf) * wide, wide), wide)
                low[:, cs] = keep[t - 1, hf] + d3[t - 1, hf].astype(F32)
                for j in range(2):
                    d1_copy(t, hf, j).wait_send()
                d2_copy(t, hf).wait_send()
                d3_copy(t, hf).wait_send()

        return carry

    lax.fori_loop(1, far + 5, down_step, 0)
    ring_end(DOWN)

    sums = [
        ALPHA * mid[hf, tp, pair].astype(F32) + low[:, hf * half : (hf + 1) * half] for hf in range(2)
    ]
    for hf, part in enumerate(layer_norm(sums, cgain_ref)):
        out_ref[:, hf * half : (hf + 1) * half] = part

    for hf in range(2):
        for j in range(2):
            b1_copy(hf, j).wait_send()
            m1_copy(hf, j).wait_send()
            m2_copy(hf, j).wait_send()
        b2_copy(hf).wait_send()
        my_copy(hf).wait_send()


def solution(mesh):
    spn, tpn = mesh.shape["sp"], mesh.shape["tp"]
    chips = spn // 2
    assert spn % 4 == 0 and tpn == 4 and mesh.shape["grp"] % 2 == 0

    def shards(res, q, k, v, f, hgain, wo, wu, wd, mgain, cgain):
        rows = q.shape[0]
        own, width = res.shape
        half = width // 2
        up_rows, ff = wu.shape
        ffh = ff // 2
        cols = wd.shape[1]
        wide = 2 * cols
        far = chips // 2
        toks = 2 * 4 * own
        f_t = jnp.pad(f.T, ((0, 4), (0, 0)))
        any_spec = pl.BlockSpec(memory_space=pl.ANY)
        vmem = pl.BlockSpec(memory_space=pltpu.VMEM)
        dma = pltpu.SemaphoreType.DMA
        return pl.pallas_call(
            functools.partial(layer_kernel, chips),
            out_shape=jax.ShapeDtypeStruct((own, width), BF16),
            in_specs=[any_spec, any_spec, any_spec, any_spec, vmem, vmem, any_spec, any_spec, any_spec, vmem, vmem],
            out_specs=vmem,
            scratch_shapes=[
                pltpu.VMEM((4, rows, HD), BF16),
                pltpu.VMEM((spn, 2, rows, HD), BF16),
                pltpu.VMEM((spn, 8, rows), F32),
                pltpu.VMEM(wo.shape, BF16),
                pltpu.VMEM((spn, up_rows, ffh), BF16),
                pltpu.VMEM((ffh, cols), BF16),
                pltpu.VMEM((spn, cols, ffh), BF16),
                pltpu.VMEM((4, rows, HD), F32),
                pltpu.VMEM((4, rows, HD), F32),
                pltpu.VMEM((4, rows, HD), F32),
                pltpu.VMEM((rows, 4 * HD), BF16),
                pltpu.VMEM((2, 4, own, half), BF16),
                pltpu.VMEM((2, 2, own, half), BF16),
                pltpu.VMEM((2, own, half), BF16),
                pltpu.VMEM((2, own, half), BF16),
                pltpu.VMEM((2, 4, 2, own, half), BF16),
                pltpu.VMEM((toks, ffh), BF16),
                pltpu.VMEM((far, 2, 4, 2, own, wide), BF16),
                pltpu.VMEM((far, 2, 2, 2, own, wide), BF16),
                pltpu.VMEM((far, 2, 2, own, wide), BF16),
                pltpu.VMEM((far, 2, 2, own, wide), BF16),
                pltpu.VMEM((far, 2, own, wide), BF16),
                pltpu.VMEM((far, 2, own, wide), BF16),
                pltpu.VMEM((far, 2, own, wide), F32),
                pltpu.VMEM((own, width), F32),
                dma((4, 2)),
                dma((4, 2, far + 1)),
                dma((4, 2)),
                dma((4, 2, far + 1)),
                dma((10,)),
                dma((2, 3)),
                dma((2, 3)),
                dma((2, 5)),
                dma((2, 5)),
                dma((far, 2, 4)),
                dma((far, 2, 4)),
            ],
            compiler_params=pltpu.CompilerParams(
                collective_id=0, has_side_effects=True, vmem_limit_bytes=56 * 1024 * 1024
            ),
            name="layer",
        )(q, k, v, f_t, res, hgain.reshape(4, HD), wo, wu, wd, mgain.reshape(1, width), cgain.reshape(1, width))

    def body(residual_in, query_rows, key_rows, value_rows, forget_cumsum, head_gain, w_out, w_up, w_down, mixer_gain, channel_gain):
        return shards(
            residual_in, query_rows, key_rows, value_rows, forget_cumsum, head_gain, w_out, w_up, w_down,
            mixer_gain, channel_gain,
        )

    placed = (
        P(("grp", "sp", "tp"), None),
        P(("grp", "sp"), "tp"),
        P(("grp", "sp"), "tp"),
        P(("grp", "sp"), "tp"),
        P(("grp", "sp"), "tp"),
        P("tp"),
        P("tp", None),
        P("sp", "tp"),
        P("tp", "sp"),
        P(),
        P(),
    )
    return jax.shard_map(
        body, mesh=mesh, in_specs=placed, out_specs=P(("grp", "sp", "tp"), None), check_vma=False
    )
```

```python
import functools

import jax
import jax.numpy as jnp
from jax import lax
from jax.experimental import pallas as pl
from jax.experimental.pallas import tpu as pltpu
from jax.sharding import PartitionSpec as P

HD = 128
ALPHA = 8.0**0.25
EPSILON = 1e-05
NEG_FILL = -1e30
LOG2E = 1.4426950408889634
MESH = pl.DeviceIdType.MESH
F32 = jnp.float32
BF16 = jnp.bfloat16

KV, GATE, UP, DOWN = (0, 1, 2, 3), (4,), (5, 6), (7, 8)


def dot_nt(a, b):
    return lax.dot_general(a, b, (((1,), (1,)), ((), ())), preferred_element_type=F32)


def dot_nn(a, b):
    return lax.dot_general(a, b, (((1,), (0,)), ((), ())), preferred_element_type=F32)


def layer_kernel(
    chips,
    q_hbm, k_hbm, v_hbm, f_hbm, res_ref, hgain_ref, wo_hbm, wu_hbm, wd_hbm, mgain_ref, cgain_ref,
    out_ref,
    q_s, kv, gate, wo_s, wu, wd, acc, m_s, l_s, heads, bp, b1, b2t, b2, mid, act,
    dp, d1, d2t, d2, d3t, d3, keep, low,
    ring_send, ring_recv, twin_send, twin_recv, local, bx_send, bx_recv, mx_send, mx_recv,
    dx_send, dx_recv,
):
    far = chips // 2
    grp, sp, tp = lax.axis_index("grp"), lax.axis_index("sp"), lax.axis_index("tp")
    z, core = sp // 2, sp % 2
    pair = grp % 2
    rows = q_s.shape[1]
    ffh = act.shape[1]
    right = (grp, ((z + 1) % chips) * 2 + core, tp)
    left = (grp, ((z + chips - 1) % chips) * 2 + core, tp)
    twin = (grp, z * 2 + 1 - core, tp)
    xa = tp + 1 - 2 * (tp % 2)
    xb = 3 - tp
    dev_a, dev_b = (grp, sp, xa), (grp, sp, xb)
    dev_y = (grp + 1 - 2 * pair, sp, tp)
    peers = (right, left, twin, dev_a, dev_b, dev_y)

    def remote(src, dst, ss, rs, dev):
        return pltpu.make_async_remote_copy(
            src_ref=src, dst_ref=dst, send_sem=ss, recv_sem=rs, device_id=dev, device_id_type=MESH
        )

    def when(cond, fn):
        if isinstance(cond, bool):
            if cond:
                fn()
        else:
            pl.when(cond)(fn)

    def both(a, b):
        return (a and b) if isinstance(a, bool) and isinstance(b, bool) else jnp.logical_and(a, b)

    def piece(st, slot):
        if st in KV:
            n = rows // 2
            return kv.at[slot, st // 2, pl.ds(st % 2 * n, n)]
        if st in GATE:
            return gate.at[slot]
        group, buf = (UP, wu) if st in UP else (DOWN, wd)
        n = buf.shape[1] // len(group)
        return buf.at[slot, pl.ds((st - group[0]) * n, n)]

    def ring_copy(st, way, slot, s):
        buf = piece(st, slot)
        return remote(buf, buf, ring_send.at[st, way], ring_recv.at[st, way, s], right if way == 0 else left)

    def twin_copy(st, way, slot, s):
        buf = piece(st, slot)
        return remote(buf, buf, twin_send.at[st, way], twin_recv.at[st, way, s], twin)

    def chip_at(way, s):
        return (z + chips - s) % chips if way == 0 else (z + s) % chips

    first_half = far - 2
    lower, top = z <= first_half, z == chips - 1

    def ring_begin(group, way):
        for st in group:
            ring_copy(st, way, sp, 1).start()

    def twin_begin(group):
        for st in group:
            twin_copy(st, 0, sp, 0).start()

    def ring_step(group, s):
        with jax.named_scope("ring%d" % group[0]):

            def one(st, way, last):
                slot = chip_at(way, s) * 2 + core
                ring_copy(st, way, slot, s).wait_recv()
                ring_copy(st, way, slot, s).wait_send()
                when(s < last, lambda: ring_copy(st, way, slot, s + 1).start())
                when(way == 0 or s > 1, lambda: twin_copy(st, way, slot, s).wait_send())
                twin_copy(st, way, slot, s).start()

            def both_ways():
                for st in group:
                    one(st, 0, far)
                    one(st, 1, far - 1)

            def one_way():
                for st in group:
                    one(st, 0, far)

            when(s < far, both_ways)
            when(s == far, one_way)

    def causal_step(group, s):
        def up(st):
            slot = chip_at(0, s) * 2 + core
            ring_copy(st, 0, slot, s).wait_recv()

            @pl.when(jnp.logical_not(top))
            def _():
                ring_copy(st, 0, slot, s).wait_send()
                when(s < far, lambda: ring_copy(st, 0, slot, s + 1).start())

            twin_copy(st, 0, slot, s).wait_send()
            twin_copy(st, 0, slot, s).start()

        def down(st):
            slot = chip_at(1, s) * 2 + core
            ring_copy(st, 1, slot, s).wait_recv()

            @pl.when(jnp.logical_or(lower, z + s > chips))
            def _():
                ring_copy(st, 1, slot, s).wait_send()

            when(s < far - 1, lambda: ring_copy(st, 1, slot, s + 1).start())

            @pl.when(z + s >= chips)
            def _():
                @pl.when(z + s > chips)
                def _():
                    twin_copy(st, 1, slot, s).wait_send()

                twin_copy(st, 1, slot, s).start()

        with jax.named_scope("kv"):

            @pl.when(z - s >= 0)
            def _():
                for st in group:
                    up(st)

            @pl.when(jnp.logical_and(s < far, jnp.logical_or(z + s <= first_half, z + s >= chips)))
            def _():
                for st in group:
                    down(st)

    def causal_wait(group, s):
        with jax.named_scope("kvtwin"):

            @pl.when(z - s >= 0)
            def _():
                for st in group:
                    twin_copy(st, 0, chip_at(0, s) * 2 + 1 - core, s).wait_recv()

            @pl.when(jnp.logical_and(s < far, z + s >= chips))
            def _():
                for st in group:
                    twin_copy(st, 1, chip_at(1, s) * 2 + 1 - core, s).wait_recv()

    def causal_end(group):
        for st in group:
            twin_copy(st, 0, sp, 0).wait_send()

        @pl.when(z < far)
        def _():
            for st in group:
                ring_copy(st, 0, sp, 1).wait_send()

        @pl.when(lower)
        def _():
            for st in group:
                ring_copy(st, 1, sp, 1).wait_send()

        @pl.when(z + far > chips)
        def _():
            for st in group:
                twin_copy(st, 1, sp, 1).wait_send()

    def twin_wait(group, s):
        with jax.named_scope("twin%d" % group[0]):
            for st in group:
                twin_copy(st, 0, chip_at(0, s) * 2 + 1 - core, s).wait_recv()

            def other():
                for st in group:
                    twin_copy(st, 1, chip_at(1, s) * 2 + 1 - core, s).wait_recv()

            when(both(s > 0, s < far), other)

    def ring_end(group):
        for st in group:
            twin_copy(st, 0, sp, 0).wait_send()
            twin_copy(st, 1, sp, 0).wait_send()

    loads = [
        pltpu.make_async_copy(k_hbm, kv.at[sp, 0], local.at[0]),
        pltpu.make_async_copy(v_hbm, kv.at[sp, 1], local.at[1]),
        pltpu.make_async_copy(f_hbm, gate.at[sp], local.at[2]),
        pltpu.make_async_copy(wu_hbm.at[:, pl.ds(pl.multiple_of(pair * ffh, ffh), ffh)], wu.at[sp], local.at[3]),
        pltpu.make_async_copy(wd_hbm.at[:, pl.ds(pl.multiple_of(pair * ffh, ffh), ffh)], wd.at[sp], local.at[4]),
        pltpu.make_async_copy(wo_hbm, wo_s, local.at[5]),
    ]
    loads += [pltpu.make_async_copy(q_hbm.at[:, pl.ds(h * HD, HD)], q_s.at[h], local.at[6 + h]) for h in range(4)]
    for c in loads:
        c.start()

    with jax.named_scope("entry"):
        barrier = pltpu.get_barrier_semaphore()
        for dev in peers:
            pl.semaphore_signal(barrier, inc=1, device_id=dev, device_id_type=MESH)
        pl.semaphore_wait(barrier, len(peers))
        for c in loads[:3]:
            c.wait()

        @pl.when(jnp.logical_not(top))
        def _():
            ring_begin(KV + GATE, 0)

        @pl.when(lower)
        def _():
            ring_begin(KV + GATE, 1)

        twin_begin(KV + GATE)
        loads[3].wait()

        @pl.when(jnp.logical_not(lower))
        def _():
            ring_begin(UP, 1)

        @pl.when(top)
        def _():
            ring_begin(UP, 0)

    gate_base = [None] * 4
    own_gate = gate[sp]
    for h in range(4):
        gate_base[h] = own_gate[h : h + 1, 0:1]

    def scores(h, src):
        s = dot_nt(q_s[h], kv[src, 0])
        bias = (gate_base[h] - gate[src][h : h + 1, :]) * LOG2E
        return s * (HD**-0.5 * LOG2E) + bias

    def spread(col):
        return jnp.broadcast_to(col, (rows, HD))

    for c in loads[6:]:
        c.wait()
    with jax.named_scope('diag'):
        causal = lax.broadcasted_iota(jnp.int32, (rows, rows), 1) <= lax.broadcasted_iota(jnp.int32, (rows, rows), 0)
        for h in range(4):
            s = jnp.where(causal, scores(h, sp), NEG_FILL)
            m = spread(jnp.max(s, axis=1, keepdims=True))
            p = jnp.exp2(s - jnp.concatenate([m] * (rows // HD), axis=1))
            m_s[h] = m
            l_s[h] = spread(jnp.sum(p, axis=1, keepdims=True))
            acc[h] = dot_nn(p.astype(BF16), kv[sp, 1])

    def attend(srcs):
        with jax.named_scope('attend'):
            attend_(srcs)

    def attend_(srcs):
        for h in range(4):
            ss = [scores(h, src) for src in srcs]
            top = functools.reduce(jnp.maximum, ss)
            m_old = m_s[h]
            m = jnp.maximum(m_old, spread(jnp.max(top, axis=1, keepdims=True)))
            wide = jnp.concatenate([m] * (rows // HD), axis=1)
            ps = [jnp.exp2(s - wide) for s in ss]
            fade = jnp.exp2(m_old - m)
            total = functools.reduce(jnp.add, ps)
            m_s[h] = m
            l_s[h] = l_s[h] * fade + spread(jnp.sum(total, axis=1, keepdims=True))
            out = dot_nn(ps[0].astype(BF16), kv[srcs[0], 1])
            for p, src in zip(ps[1:], srcs[1:]):
                out = out + dot_nn(p.astype(BF16), kv[src, 1])
            acc[h] = acc[h] * fade + out

    def attend_step(s):
        @pl.when(z - s >= 0)
        def _():
            c = chip_at(0, s) * 2
            attend([c, c + 1])

        @pl.when(jnp.logical_and(s < far, z + s >= chips))
        def _():
            c = chip_at(1, s) * 2
            attend([c, c + 1])

    def kv_step(s, carry):
        causal_step(KV + GATE, s)
        causal_wait(KV + GATE, s - 1)

        @pl.when(jnp.logical_and(s == 1, core == 1))
        def _():
            attend([sp - 1])

        @pl.when(s > 1)
        def _():
            attend_step(s - 1)

        return carry

    lax.fori_loop(1, far + 1, kv_step, 0)

    @pl.when(lower)
    def _():
        ring_begin(UP, 1)

    @pl.when(jnp.logical_not(top))
    def _():
        ring_begin(UP, 0)

    twin_begin(UP)
    causal_wait(KV + GATE, far)
    attend_step(far)
    causal_end(KV + GATE)

    loads[4].wait()
    cols = wd.shape[1]

    loads[5].wait()
    with jax.named_scope('headnorm'):
        for h in range(4):
            att = acc[h] / l_s[h]
            norm = lax.rsqrt(jnp.mean(att * att, axis=1, keepdims=True) + EPSILON)
            heads[:, h * HD : (h + 1) * HD] = (att * norm * hgain_ref[h : h + 1, :]).astype(BF16)
    half = bp.shape[3]
    own = bp.shape[2]
    with jax.named_scope('wout'):
        for j in range(4):
            w = half // 2
            part = dot_nn(heads[...], wo_s[:, j * w : (j + 1) * w]).astype(BF16)
            bp[j // 2, :, :, (j % 2) * w : (j % 2 + 1) * w] = part.reshape(4, own, w)

    far_a = 3 - xa
    first = (dev_a, dev_b)
    second = (dev_b, dev_a)
    first_x = (xa, xb)
    second_x = (xb, xa)

    def b1_copy(hf, j):
        src = bp.at[hf, first_x[hf] if j == 0 else far_a]
        return remote(src, b1.at[hf, j], bx_send.at[hf, j], bx_recv.at[hf, j], first[hf])

    def b2_copy(hf):
        return remote(b2t.at[hf], b2.at[hf], bx_send.at[hf, 2], bx_recv.at[hf, 2], second[hf])

    for hf in range(2):
        b1_copy(hf, 1).start()
    for hf in range(2):
        b1_copy(hf, 0).start()
    ring_step(UP, 1)
    with jax.named_scope('b1'):
        for hf in range(2):
            b1_copy(hf, 1).wait_recv()
            b2t[hf] = (bp[hf, second_x[hf]].astype(F32) + b1[hf, 1].astype(F32)).astype(BF16)
            b2_copy(hf).start()
    ring_step(UP, 2)
    sums = []
    with jax.named_scope('b1w'):
        for hf in range(2):
            b1_copy(hf, 0).wait_recv()
    ring_step(UP, 3)
    with jax.named_scope('b2'):
        for hf in range(2):
            b2_copy(hf).wait_recv()
            part = bp[hf, tp].astype(F32) + b1[hf, 0].astype(F32) + b2[hf].astype(F32)
            sums.append(ALPHA * res_ref[:, hf * half : (hf + 1) * half].astype(F32) + part)

    def layer_norm(parts, gain_ref):
        width = 2 * half
        mean = sum(jnp.sum(p, axis=1, keepdims=True) for p in parts) * (1.0 / width)
        parts = [p - mean for p in parts]
        var = sum(jnp.sum(p * p, axis=1, keepdims=True) for p in parts) * (1.0 / width)
        inv = lax.rsqrt(var + EPSILON)
        return [
            (p * inv * gain_ref[:, i * half : (i + 1) * half]).astype(BF16) for i, p in enumerate(parts)
        ]

    with jax.named_scope('ln1'):
        for hf, part in enumerate(layer_norm(sums, mgain_ref)):
            mid[hf, tp, pair] = part

    def my_copy(hf):
        return remote(mid.at[hf, tp, pair], mid.at[hf, tp, pair], mx_send.at[hf, 0], mx_recv.at[hf, 0], dev_y)

    def m1_copy(hf, j):
        ref = mid.at[hf, tp, pair if j == 0 else 1 - pair]
        return remote(ref, ref, mx_send.at[hf, 1 + j], mx_recv.at[hf, 1 + j], first[hf])

    def m2_copy(hf, j):
        ref = mid.at[hf, tp if j == 0 else first_x[hf]]
        return remote(ref, ref, mx_send.at[hf, 3 + j], mx_recv.at[hf, 3 + j], second[hf])

    for hf in range(2):
        my_copy(hf).start()
        m1_copy(hf, 0).start()
    ring_step(UP, 4)
    with jax.named_scope('my'):
        for hf in range(2):
            my_copy(hf).wait_recv()
            m1_copy(hf, 1).start()
            m2_copy(hf, 0).start()
    ring_step(UP, 5)
    ring_step(UP, 6)
    for way in range(2):
        ring_begin(DOWN, way)
    twin_begin(DOWN)
    with jax.named_scope('m1'):
        for hf in range(2):
            m1_copy(hf, 0).wait_recv()
            m1_copy(hf, 1).wait_recv()
            m2_copy(hf, 1).start()
    ring_step(UP, 7)
    ring_step(UP, 8)
    for s in range(far + 1):
        twin_wait(UP, s)
    ring_step(DOWN, 1)
    ring_step(DOWN, 2)
    with jax.named_scope('m2'):
        for hf in range(2):
            m2_copy(hf, 0).wait_recv()
            m2_copy(hf, 1).wait_recv()
    ring_end(UP)

    toks = act.shape[0]
    tile = 256

    def up_tile(j, carry):
        cs = pl.ds(pl.multiple_of(j * tile, tile), tile)
        total = None
        for hf in range(2):
            blocks = wu.shape[0] // 2
            w = wu[hf * blocks : (hf + 1) * blocks, :, cs].reshape(half, tile)
            part = dot_nn(mid[hf].reshape(toks, half), w)
            total = part if total is None else total + part
        pos = jnp.maximum(total, 0.0)
        act[:, cs] = (pos * pos).astype(BF16)
        return carry

    with jax.named_scope('up'):
        lax.fori_loop(0, ffh // tile // 2, up_tile, 0)
    ring_step(DOWN, 3)
    with jax.named_scope('up'):
        lax.fori_loop(ffh // tile // 2, ffh // tile, up_tile, 0)
    early = 3

    wide = 2 * cols

    def chunk_chip(t, hf):
        return jnp.where(t == far, z, chip_at(0, t)) if hf == 0 else jnp.where(t == far, chip_at(0, t), chip_at(1, t))

    def d1_copy(t, hf, j):
        src = dp.at[t - 1, hf, first_x[hf] if j == 0 else far_a]
        return remote(src, d1.at[t - 1, hf, j], dx_send.at[t - 1, hf, j], dx_recv.at[t - 1, hf, j], first[hf])

    def d2_copy(t, hf):
        return remote(
            d2t.at[t - 1, hf], d2.at[t - 1, hf], dx_send.at[t - 1, hf, 2], dx_recv.at[t - 1, hf, 2], second[hf]
        )

    def d3_copy(t, hf):
        return remote(
            d3t.at[t - 1, hf], d3.at[t - 1, hf], dx_send.at[t - 1, hf, 3], dx_recv.at[t - 1, hf, 3], dev_y
        )

    def down_step(i, carry):
        @pl.when(jnp.logical_and(i > early, i <= far))
        def _():
            ring_step(DOWN, i)

        @pl.when(jnp.logical_and(i >= 2, i <= far + 1))
        def _():
            t = i - 1
            twin_wait(DOWN, t)

            @pl.when(t == far)
            def _():
                twin_wait(DOWN, 0)

            with jax.named_scope('down'):
                w = jnp.concatenate(
                    [wd[pl.ds(chunk_chip(t, hf) * 2, 2)].reshape(wide, ffh) for hf in range(2)], axis=0
                )
                part = dot_nt(act[...], w).astype(BF16)
                for hf in range(2):
                    dp[t - 1, hf] = part[:, hf * wide : (hf + 1) * wide].reshape(4, 2, own, wide)
                    d1_copy(t, hf, 1).start()
                    d1_copy(t, hf, 0).start()

        @pl.when(jnp.logical_and(i >= 3, i <= far + 2))
        def _():
            with jax.named_scope('d1'):
                t = i - 2
                for hf in range(2):
                    d1_copy(t, hf, 1).wait_recv()
                    d2t[t - 1, hf] = (
                        dp[t - 1, hf, second_x[hf]].astype(F32) + d1[t - 1, hf, 1].astype(F32)
                    ).astype(BF16)
                    d2_copy(t, hf).start()

        @pl.when(jnp.logical_and(i >= 4, i <= far + 3))
        def _():
            with jax.named_scope('d2'):
                t = i - 3
                for hf in range(2):
                    d1_copy(t, hf, 0).wait_recv()
                    d2_copy(t, hf).wait_recv()

                    def whole(y):
                        return (
                            dp[t - 1, hf, tp, y].astype(F32)
                            + d1[t - 1, hf, 0, y].astype(F32)
                            + d2[t - 1, hf, y].astype(F32)
                        )

                    d3t[t - 1, hf] = whole(1 - pair).astype(BF16)
                    d3_copy(t, hf).start()
                    keep[t - 1, hf] = whole(pair)

        @pl.when(i >= 5)
        def _():
            with jax.named_scope('d3'):
                t = i - 4
                for hf in range(2):
                    d3_copy(t, hf).wait_recv()
                    cs = pl.ds(pl.multiple_of(chunk_chip(t, hf) * wide, wide), wide)
                    low[:, cs] = keep[t - 1, hf] + d3[t - 1, hf].astype(F32)
                    for j in range(2):
                        d1_copy(t, hf, j).wait_send()
                    d2_copy(t, hf).wait_send()
                    d3_copy(t, hf).wait_send()

        return carry

    lax.fori_loop(1, far + 5, down_step, 0)
    ring_end(DOWN)

    with jax.named_scope('ln2'):
        sums = [
            ALPHA * mid[hf, tp, pair].astype(F32) + low[:, hf * half : (hf + 1) * half] for hf in range(2)
        ]
        for hf, part in enumerate(layer_norm(sums, cgain_ref)):
            out_ref[:, hf * half : (hf + 1) * half] = part

    for hf in range(2):
        for j in range(2):
            b1_copy(hf, j).wait_send()
            m1_copy(hf, j).wait_send()
            m2_copy(hf, j).wait_send()
        b2_copy(hf).wait_send()
        my_copy(hf).wait_send()


def solution(mesh):
    spn, tpn = mesh.shape["sp"], mesh.shape["tp"]
    chips = spn // 2
    assert spn % 4 == 0 and tpn == 4 and mesh.shape["grp"] % 2 == 0

    def shards(res, q, k, v, f, hgain, wo, wu, wd, mgain, cgain):
        rows = q.shape[0]
        own, width = res.shape
        half = width // 2
        up_rows, ff = wu.shape
        ffh = ff // 2
        cols = wd.shape[1]
        wide = 2 * cols
        far = chips // 2
        toks = 2 * 4 * own
        any_spec = pl.BlockSpec(memory_space=pl.ANY)
        vmem = pl.BlockSpec(memory_space=pltpu.VMEM)
        dma = pltpu.SemaphoreType.DMA
        return pl.pallas_call(
            functools.partial(layer_kernel, chips),
            out_shape=jax.ShapeDtypeStruct((own, width), BF16),
            in_specs=[any_spec, any_spec, any_spec, any_spec, vmem, vmem, any_spec, any_spec, any_spec, vmem, vmem],
            out_specs=vmem,
            scratch_shapes=[
                pltpu.VMEM((4, rows, HD), BF16),
                pltpu.VMEM((spn, 2, rows, HD), BF16),
                pltpu.VMEM((spn, 4, rows), F32),
                pltpu.VMEM(wo.shape, BF16),
                pltpu.VMEM((spn, up_rows, ffh), BF16),
                pltpu.VMEM((spn, cols, ffh), BF16),
                pltpu.VMEM((4, rows, HD), F32),
                pltpu.VMEM((4, rows, HD), F32),
                pltpu.VMEM((4, rows, HD), F32),
                pltpu.VMEM((rows, 4 * HD), BF16),
                pltpu.VMEM((2, 4, own, half), BF16),
                pltpu.VMEM((2, 2, own, half), BF16),
                pltpu.VMEM((2, own, half), BF16),
                pltpu.VMEM((2, own, half), BF16),
                pltpu.VMEM((2, 4, 2, own, half), BF16),
                pltpu.VMEM((toks, ffh), BF16),
                pltpu.VMEM((far, 2, 4, 2, own, wide), BF16),
                pltpu.VMEM((far, 2, 2, 2, own, wide), BF16),
                pltpu.VMEM((far, 2, 2, own, wide), BF16),
                pltpu.VMEM((far, 2, 2, own, wide), BF16),
                pltpu.VMEM((far, 2, own, wide), BF16),
                pltpu.VMEM((far, 2, own, wide), BF16),
                pltpu.VMEM((far, 2, own, wide), F32),
                pltpu.VMEM((own, width), F32),
                dma((9, 2)),
                dma((9, 2, far + 1)),
                dma((9, 2)),
                dma((9, 2, far + 1)),
                dma((10,)),
                dma((2, 3)),
                dma((2, 3)),
                dma((2, 5)),
                dma((2, 5)),
                dma((far, 2, 4)),
                dma((far, 2, 4)),
            ],
            compiler_params=pltpu.CompilerParams(
                collective_id=0, has_side_effects=True, vmem_limit_bytes=56 * 1024 * 1024
            ),
            name="layer",
        )(q, k, v, f.T, res, hgain.reshape(4, HD), wo, wu, wd.T, mgain.reshape(1, width), cgain.reshape(1, width))

    def body(residual_in, query_rows, key_rows, value_rows, forget_cumsum, head_gain, w_out, w_up, w_down, mixer_gain, channel_gain):
        return shards(
            residual_in, query_rows, key_rows, value_rows, forget_cumsum, head_gain, w_out, w_up, w_down,
            mixer_gain, channel_gain,
        )

    placed = (
        P(("grp", "sp", "tp"), None),
        P(("grp", "sp"), "tp"),
        P(("grp", "sp"), "tp"),
        P(("grp", "sp"), "tp"),
        P(("grp", "sp"), "tp"),
        P("tp"),
        P("tp", None),
        P("sp", "tp"),
        P("tp", "sp"),
        P(),
        P(),
    )
    return jax.shard_map(
        body, mesh=mesh, in_specs=placed, out_specs=P(("grp", "sp", "tp"), None), check_vma=False
    )
```
